32 devices in a mesh: fs: 8 (over z, y), tp: 4 (over x, core).
Axes of the slice: x: 2, y: 2, z: 4, core: 2. Of those that a mesh axis runs over, the one named last changes fastest.
Arguments:
- hidden_in: bfloat16 [512, 4096], P(None, 'tp'), may hold values from -6 to 6
- up_act: bfloat16 [512, 12288], P('tp', 'fs'), may hold values from -6 to 6
- up_val: bfloat16 [512, 12288], P('tp', 'fs'), may hold values from -6 to 6
- cotangent: bfloat16 [512, 4096], P('tp'), may hold values from -6 to 6
- w_act: bfloat16 [4096, 12288], P('tp', 'fs'), may hold values from -0.09375 to 0.09375
- w_val: bfloat16 [4096, 12288], P('tp', 'fs'), may hold values from -0.09375 to 0.09375
- w_down: bfloat16 [12288, 4096], P('fs', 'tp'), may hold values from -0.0546875 to 0.0546875
- conv_act: bfloat16 [3, 12288], P(None, 'fs'), may hold values from -3 to 3
- conv_val: bfloat16 [3, 12288], P(None, 'fs'), may hold values from -3 to 3
- bias_act: bfloat16 [12288], P('fs'), may hold values from -3 to 3
- bias_val: bfloat16 [12288], P('fs'), may hold values from -3 to 3
Outputs:
- grad_input: bfloat16 [512, 4096], P(('tp', 'fs'))
- grad_w_act: float32 [4096, 12288], P('tp', 'fs')
- grad_w_val: float32 [4096, 12288], P('tp', 'fs')
- grad_w_down: float32 [12288, 4096], P('fs', 'tp')
- grad_conv_act: float32 [3, 12288], P(None, 'fs')
- grad_conv_val: float32 [3, 12288], P(None, 'fs')
- grad_bias_act: float32 [12288], P('fs')
- grad_bias_val: float32 [12288], P('fs')
- rows_act: float32 [4096], P('tp')
- rows_val: float32 [4096], P('tp')
- rows_down: float32 [12288], P('fs')
- conv_rows: float32 [2, 3], replicated
The draws below stay inside these ranges and needn't reach their ends.
All inputs are finite; a program needn't handle non-finite values.
Results may differ from the reference program's by a relative error of at most 0.0057.
Values may be sent and summed in bfloat16 or wider, within the bound.
No kernel may reach another device: no remote copies, remote signals or barrier semaphores. Data moves between devices by JAX's collectives and lax.ppermute only.
A program may use at most 128 MiB of HBM per device.

```python
import jax
import jax.numpy as jnp
from jax import lax

D = 4096
FF = 12288
KW = 3
TOKENS = 512


def with_spikes(result, own_key, source, target, parts, factor):
    owner, partner = [(jnp.arange(result.shape[axis_at]) // (result.shape[axis_at] // parts)).reshape([-1 if axis == axis_at else 1 for axis in range(result.ndim)]) for axis_at in (source, target)]
    chosen = jax.random.permutation(own_key, parts)[partner]
    strong = (owner == chosen) | (owner == (partner + parts // 2) % parts)
    return jnp.where(strong, factor * result, result)


def shard_levels(own_key, shape, cuts, smallest, top_value):
    level = 1.0
    for axis_at, parts in cuts:
        draws = jax.random.uniform(jax.random.fold_in(jax.random.fold_in(own_key, 6), axis_at), (parts,), jnp.float32, smallest / len(cuts), top_value / len(cuts))
        level = level * jnp.repeat(jnp.exp(draws), shape[axis_at] // parts).reshape((-1,) + (1,) * (len(shape) - 1 - axis_at))
    return level


def bell_draw(own_key, extent, deviation, bound, pieces=(), held_as=jnp.bfloat16):
    values = deviation * jax.random.normal(own_key, extent, jnp.float32)
    if pieces:
        values = values * shard_levels(own_key, extent, pieces, -0.22, 0.18)
    return jnp.clip(values, -bound, bound).astype(held_as)


def noise_with(own_key, dims, scale, most, cuts, heavy, dtype=jnp.bfloat16):
    entries = scale * jax.random.normal(own_key, dims, jnp.float32)
    if cuts:
        entries = entries * shard_levels(own_key, dims, cuts, -0.22, 0.18)
    return jnp.clip(with_spikes(entries, jax.random.fold_in(own_key, 3), *heavy), -most, most).astype(dtype)


def setup_inputs(seed: int = 0) -> dict:
    key_of = jax.random.split(jax.random.key(seed), 12)
    return {
        "hidden_in": bell_draw(key_of[0], (TOKENS, D), 1.0, 6.0, ((1, 4),)),
        "up_act": bell_draw(key_of[1], (TOKENS, FF), 1.0, 6.0, ((0, 4), (1, 8))),
        "up_val": bell_draw(key_of[2], (TOKENS, FF), 1.0, 6.0, ((0, 4), (1, 8))),
        "cotangent": noise_with(key_of[3], (TOKENS, D), 1.0, 6.0, ((0, 4),), (0, 1, 4, 2.0)),
        "w_act": bell_draw(key_of[4], (D, FF), D ** -0.5, 0.09375, ((0, 4), (1, 8))),
        "w_val": bell_draw(key_of[5], (D, FF), D ** -0.5, 0.09375, ((0, 4), (1, 8))),
        "w_down": bell_draw(key_of[6], (FF, D), FF ** -0.5, 0.0546875, ((0, 8), (1, 4))),
        "conv_act": bell_draw(key_of[7], (KW, FF), 0.577, 3.0, ((1, 8),)),
        "conv_val": bell_draw(key_of[8], (KW, FF), 0.577, 3.0, ((1, 8),)),
        "bias_act": bell_draw(key_of[9], (FF,), 0.5, 3.0, ((0, 8),)),
        "bias_val": bell_draw(key_of[10], (FF,), 0.5, 3.0, ((0, 8),)),
    }


def conv_ahead(upper, taps, bias):
    length = upper.shape[0]
    padded = jnp.concatenate([jnp.zeros((KW - 1, upper.shape[1]), jnp.float32), upper.astype(jnp.float32)], 0)
    total = jnp.zeros(upper.shape, jnp.float32) + bias.astype(jnp.float32)
    for offset in range(KW):
        total = total + taps[offset].astype(jnp.float32) * padded[offset:offset + length]
    return (total, padded)

def conv_behind(grad_pre, taps):
    length = grad_pre.shape[0]
    padded = jnp.concatenate([grad_pre, jnp.zeros((KW - 1, grad_pre.shape[1]), jnp.float32)], 0)
    total = jnp.zeros(grad_pre.shape, jnp.float32)
    for offset in range(KW):
        total = total + taps[offset].astype(jnp.float32) * padded[KW - 1 - offset:KW - 1 - offset + length]
    return total.astype(jnp.bfloat16)

def tap_grads(grad_pre, padded):
    length = grad_pre.shape[0]
    rows = [lax.optimization_barrier(jnp.sum(grad_pre * padded[offset:offset + length], axis=0)) for offset in range(KW)]
    return (jnp.stack(rows, 0), lax.optimization_barrier(jnp.sum(grad_pre, axis=0)))

def reference(hidden_in, up_act, up_val, cotangent, w_act, w_val, w_down, conv_act, conv_val, bias_act, bias_val):
    pre_act, padded_act = conv_ahead(up_act, conv_act, bias_act)
    pre_val, padded_val = conv_ahead(up_val, conv_val, bias_val)
    gelu_act, gelu_back = jax.vjp(jax.nn.gelu, pre_act)
    mixed = (gelu_act * pre_val).astype(jnp.bfloat16)
    grad_mixed = jnp.dot(cotangent, w_down.T, preferred_element_type=jnp.float32).astype(jnp.bfloat16)
    grad_mixed = lax.optimization_barrier(grad_mixed).astype(jnp.float32)
    grad_pre_act = gelu_back(grad_mixed * pre_val)[0]
    grad_pre_val = grad_mixed * gelu_act
    grad_up_act = conv_behind(grad_pre_act, conv_act)
    grad_up_val = conv_behind(grad_pre_val, conv_val)
    grad_conv_act, grad_bias_act = tap_grads(grad_pre_act, padded_act)
    grad_conv_val, grad_bias_val = tap_grads(grad_pre_val, padded_val)
    grad_w_act = jnp.dot(hidden_in.T, grad_up_act, preferred_element_type=jnp.float32)
    grad_w_val = jnp.dot(hidden_in.T, grad_up_val, preferred_element_type=jnp.float32)
    grad_w_down = jnp.dot(mixed.T, cotangent, preferred_element_type=jnp.float32)
    grad_input = jnp.dot(grad_up_act, w_act.T, preferred_element_type=jnp.float32)
    grad_input = grad_input + jnp.dot(grad_up_val, w_val.T, preferred_element_type=jnp.float32)
    grad_input = grad_input.astype(jnp.bfloat16)
    rows_act = lax.optimization_barrier(jnp.sum(grad_w_act * grad_w_act, axis=1))
    rows_val = lax.optimization_barrier(jnp.sum(grad_w_val * grad_w_val, axis=1))
    rows_down = lax.optimization_barrier(jnp.sum(grad_w_down * grad_w_down, axis=1))
    conv_rows = jnp.stack([lax.optimization_barrier(jnp.sum(grad_conv_act * grad_conv_act, axis=1)), lax.optimization_barrier(jnp.sum(grad_conv_val * grad_conv_val, axis=1))], 0)
    return (grad_input, grad_w_act, grad_w_val, grad_w_down, grad_conv_act, grad_conv_val, grad_bias_act, grad_bias_val, rows_act, rows_val, rows_down, conv_rows)
```

```python
import functools

import jax
import jax.numpy as jnp
from jax import lax
from jax.experimental import pallas as pl
from jax.experimental.pallas import tpu as pltpu
from jax.sharding import PartitionSpec as P

F32 = jnp.float32
BF16 = jnp.bfloat16
GELU_SCALE = 0.7978845608028654
GELU_CUBIC = 0.044715


def contract(left, right, dims, precision=None):
    return lax.dot_general(
        left, right, ((dims[:1], dims[1:]), ((), ())), precision=precision, preferred_element_type=F32
    )


def tile_of(size, wanted):
    return wanted if size % wanted == 0 else size


def chunk_of(rows):
    return 64 if rows % 64 == 0 else rows


def call(kernel, grid, in_specs, out_specs, out_shape, scratch=(), flops=0):
    return pl.pallas_call(
        kernel,
        grid=grid,
        in_specs=in_specs,
        out_specs=out_specs,
        out_shape=out_shape,
        scratch_shapes=scratch,
        cost_estimate=pl.CostEstimate(flops=flops, transcendentals=0, bytes_accessed=flops // 256),
        compiler_params=pltpu.CompilerParams(
            dimension_semantics=("arbitrary",), vmem_limit_bytes=48 * 1024 * 1024
        ),
    )


def shifted_back(ref, start, rows, reach):
    current = ref[start : start + rows, :].astype(F32)
    if start == 0:
        before = jnp.zeros((8, current.shape[1]), F32)
    else:
        before = ref[start - 16 : start, :].astype(F32)[8:]
    joined = jnp.concatenate([before, current], 0)
    return [joined[8 - reach + k : 8 - reach + k + rows] for k in range(reach)] + [current]


def forward_kernel(up_act, up_val, conv_act, conv_val, bias_act, bias_val, mixed, slope, gate):
    total = up_act.shape[0]
    reach = conv_act.shape[0] - 1
    rows = chunk_of(total)

    def conv(ref, taps, bias, start):
        value = bias[...].astype(F32)
        weights = taps[...].astype(F32)
        for k, shifted in enumerate(shifted_back(ref, start, rows, reach)):
            value = value + weights[k : k + 1] * shifted
        return value

    for start in range(0, total, rows):
        here = slice(start, start + rows)
        act = conv(up_act, conv_act, bias_act, start)
        val = conv(up_val, conv_val, bias_val, start)
        square = act * act
        bent = jnp.tanh(act * (GELU_SCALE + (GELU_SCALE * GELU_CUBIC) * square))
        half = 0.5 + 0.5 * bent
        gelu = act * half
        inner = GELU_SCALE + (3.0 * GELU_SCALE * GELU_CUBIC) * square
        back = half + 0.5 * act * (1.0 - bent * bent) * inner
        mixed[here, :] = (gelu * val).astype(BF16)
        slope[here, :] = back * val
        gate[here, :] = gelu


def backward_kernel(
    core, mine, theirs, slope, gate, up_act, up_val, conv_act, conv_val, w_act, w_val,
    grad_act, grad_val, stats, partial, acc, *, tp_count, fs_count,
):
    total = up_act.shape[0]
    half = total // 2
    reach = conv_act.shape[0] - 1
    rows = chunk_of(half)
    first = core[0] == 0

    def mixed_grad(start, count):
        low = start < half
        at = slice(start % half, start % half + count)
        own, other = mine[at, :], theirs[at, :]
        own, other = own.astype(F32), other.astype(F32)
        return jnp.where(first == low, own, other)

    weights = (conv_act[...].astype(F32), conv_val[...].astype(F32))
    sums = [[None] * (reach + 2), [None] * (reach + 2)]

    def fold(value):
        if rows % 8 == 0:
            return jnp.sum(value.reshape(rows // 8, 8, value.shape[1]), axis=0)
        return jnp.sum(value, axis=0, keepdims=True)

    for start in range(0, total, rows):
        here = slice(start, start + rows)
        grad = mixed_grad(start, rows)
        last = start + rows >= total
        if not last:
            grad_next = mixed_grad(start + rows, 16)[:8]
        for role, (factor, up, out) in enumerate(
            ((slope, up_act, grad_act), (gate, up_val, grad_val))
        ):
            pre = grad * factor[here, :]
            if last:
                after = jnp.zeros((8, pre.shape[1]), F32)
            else:
                after = grad_next * factor[start + rows : start + rows + 8, :]
            joined = jnp.concatenate([pre, after], 0)
            source = up[here, :].astype(F32)
            value = None
            for k in range(reach + 1):
                ahead = reach - k
                moved = joined[ahead : ahead + rows] if ahead else pre
                term = weights[role][k : k + 1] * moved
                value = term if value is None else value + term
                add = fold(moved * source)
                sums[role][k] = add if sums[role][k] is None else sums[role][k] + add
            add = fold(pre)
            sums[role][-1] = add if sums[role][-1] is None else sums[role][-1] + add
            out[here, :] = value.astype(BF16)
    lines = [jnp.sum(entry, axis=0, keepdims=True) for role in sums for entry in role]
    for index, line in enumerate(lines):
        stats[index : index + 1, :] = line

    product = contract(grad_act[...], w_act[...], (1, 1)) + contract(
        grad_val[...], w_val[...], (1, 1)
    )
    step = pl.program_id(0)

    @pl.when(step == 0)
    def _():
        acc[...] = product

    @pl.when(step > 0)
    def _():
        acc[...] += product

    @pl.when(step == pl.num_programs(0) - 1)
    def _():
        shard = total // (tp_count * fs_count)
        for f in range(fs_count):
            for i in range(tp_count):
                start = (i * fs_count + f) * shard
                partial[f, i * shard : (i + 1) * shard, :] = acc[start : start + shard, :].astype(BF16)


def weight_kernel(left, *refs):
    count = len(refs) // 3
    for right, out, squares in zip(refs[:count], refs[count : 2 * count], refs[2 * count :]):
        value = contract(left[...], right[...], (0, 0))
        out[...] = value
        value = value * value
        width = value.shape[1]
        if width % 128 == 0:
            value = functools.reduce(
                jnp.add, [value[:, at : at + 128] for at in range(0, width, 128)]
            )
        ones = jnp.ones((8, value.shape[1]), F32)
        squares[...] = contract(ones, value, (1, 1), lax.Precision.HIGHEST)[:1]


def weight_grads(left, rights):
    rows, height = left.shape
    tile = tile_of(height, 256)
    width = rights[0].shape[1]
    count = len(rights)
    out = call(
        weight_kernel,
        (height // tile,),
        [pl.BlockSpec((rows, tile), lambda i: (0, i))]
        + [pl.BlockSpec((rows, width), lambda i: (0, 0))] * count,
        [pl.BlockSpec((tile, width), lambda i: (i, 0))] * count
        + [pl.BlockSpec((1, tile), lambda i: (0, i))] * count,
        [jax.ShapeDtypeStruct((height, width), F32)] * count
        + [jax.ShapeDtypeStruct((1, height), F32)] * count,
        flops=2 * rows * height * width * count,
    )(left, *rights)
    return out[:count], [entry.reshape(height) for entry in out[count:]]


def per_device(
    hidden_in,
    up_act,
    up_val,
    cotangent,
    w_act,
    w_val,
    w_down,
    conv_act,
    conv_val,
    bias_act,
    bias_val,
):
    local_rows = cotangent.shape[0]
    tap_count = conv_act.shape[0]
    tp_count = lax.axis_size("tp")
    fs_count = lax.axis_size("fs")
    chips = tp_count // 2
    total = local_rows * tp_count
    half = total // 2
    units = up_act.shape[1]
    width = w_act.shape[0]
    core = lax.axis_index("tp") % 2
    swap_cores = [(i, i ^ 1) for i in range(tp_count)]

    all_act = lax.all_gather(up_act, "tp", axis=0, tiled=True)
    all_val = lax.all_gather(up_val, "tp", axis=0, tiled=True)
    cot_blocks = jnp.transpose(cotangent.reshape(local_rows, tp_count, width), (1, 0, 2))
    cot_columns = lax.all_to_all(cot_blocks, "tp", split_axis=0, concat_axis=0, tiled=True)
    cot_columns = cot_columns.reshape(total, width)

    tile = tile_of(units, 256)
    column = pl.BlockSpec((total, tile), lambda i: (0, i))
    taps_spec = pl.BlockSpec((tap_count, tile), lambda i: (0, i))
    line_spec = pl.BlockSpec((1, tile), lambda i: (0, i))
    mixed, slope, gate = call(
        forward_kernel,
        (units // tile,),
        [column, column, taps_spec, taps_spec, line_spec, line_spec],
        [column] * 3,
        [
            jax.ShapeDtypeStruct((total, units), BF16),
            jax.ShapeDtypeStruct((total, units), F32),
            jax.ShapeDtypeStruct((total, units), F32),
        ],
        flops=60 * total * units,
    )(all_act, all_val, conv_act, conv_val, bias_act.reshape(1, units), bias_val.reshape(1, units))

    away = contract(
        lax.dynamic_slice_in_dim(cot_columns, (1 - core) * half, half, 0), w_down, (1, 1)
    ).astype(BF16)
    arrived = lax.ppermute(away, "tp", swap_cores)
    kept = contract(lax.dynamic_slice_in_dim(cot_columns, core * half, half, 0), w_down, (1, 1))
    chip_sum = (kept + arrived.astype(F32)).astype(BF16)
    if chips == 2:
        other = lax.ppermute(chip_sum, "tp", [(i, (i + 2) % tp_count) for i in range(tp_count)])
        mine = (chip_sum.astype(F32) + other.astype(F32)).astype(BF16)
    else:
        groups = [list(range(c, tp_count, 2)) for c in range(2)]
        parts = lax.all_gather(chip_sum, "tp", axis=0, axis_index_groups=groups)
        mine = jnp.sum(parts.astype(F32), axis=0).astype(BF16)
    theirs = lax.ppermute(mine, "tp", swap_cores)

    (grad_w_down,), (down_squares,) = weight_grads(mixed, (cot_columns,))

    shard = local_rows // fs_count
    half_spec = pl.BlockSpec((half, tile), lambda i: (0, i))
    weight_spec = pl.BlockSpec((width, tile), lambda i: (0, i))
    stat_count = 2 * (tap_count + 1)
    grad_act, grad_val, stats, partial = call(
        functools.partial(backward_kernel, tp_count=tp_count, fs_count=fs_count),
        (units // tile,),
        [pl.BlockSpec(memory_space=pltpu.SMEM)]
        + [half_spec] * 2
        + [column] * 4
        + [taps_spec] * 2
        + [weight_spec] * 2,
        [
            column,
            column,
            pl.BlockSpec((stat_count, tile), lambda i: (0, i)),
            pl.BlockSpec((fs_count, tp_count * shard, width), lambda i: (0, 0, 0)),
        ],
        [
            jax.ShapeDtypeStruct((total, units), BF16),
            jax.ShapeDtypeStruct((total, units), BF16),
            jax.ShapeDtypeStruct((stat_count, units), F32),
            jax.ShapeDtypeStruct((fs_count, tp_count * shard, width), BF16),
        ],
        scratch=[pltpu.VMEM((total, width), F32)],
        flops=4 * total * units * width,
    )(
        core.reshape(1).astype(jnp.int32),
        mine,
        theirs,
        slope,
        gate,
        all_act,
        all_val,
        conv_act,
        conv_val,
        w_act,
        w_val,
    )
    pieces = lax.all_to_all(partial, "fs", split_axis=0, concat_axis=0, tiled=True)
    (grad_w_act, grad_w_val), (act_squares, val_squares) = weight_grads(
        hidden_in, (grad_act, grad_val)
    )
    taps_act, sums_act = stats[:tap_count], stats[tap_count]
    taps_val, sums_val = stats[tap_count + 1 : 2 * tap_count + 1], stats[2 * tap_count + 1]
    tap_squares = jnp.stack(
        [jnp.sum(taps_act * taps_act, axis=1), jnp.sum(taps_val * taps_val, axis=1)], 0
    )
    rows_down = lax.psum(down_squares, "tp")
    rows_act, rows_val, conv_rows = lax.psum((act_squares, val_squares, tap_squares), "fs")
    summed = jnp.sum(pieces.astype(F32), axis=0).astype(BF16).reshape(tp_count, shard, width)
    blocks = lax.all_to_all(summed, "tp", split_axis=0, concat_axis=0, tiled=True)
    grad_input = jnp.transpose(blocks, (1, 0, 2)).reshape(shard, tp_count * width)
    return (
        grad_input,
        grad_w_act,
        grad_w_val,
        grad_w_down,
        taps_act,
        taps_val,
        sums_act,
        sums_val,
        rows_act,
        rows_val,
        rows_down,
        conv_rows,
    )


def solution(mesh):
    return jax.shard_map(
        per_device,
        mesh=mesh,
        in_specs=(
            P(None, "tp"),
            P("tp", "fs"),
            P("tp", "fs"),
            P("tp", None),
            P("tp", "fs"),
            P("tp", "fs"),
            P("fs", "tp"),
            P(None, "fs"),
            P(None, "fs"),
            P("fs"),
            P("fs"),
        ),
        out_specs=(
            P(("tp", "fs"), None),
            P("tp", "fs"),
            P("tp", "fs"),
            P("fs", "tp"),
            P(None, "fs"),
            P(None, "fs"),
            P("fs"),
            P("fs"),
            P("tp"),
            P("tp"),
            P("fs"),
            P(),
        ),
        check_vma=False,
    )
```

```python
import functools

import jax
import jax.numpy as jnp
from jax import lax
from jax.experimental import pallas as pl
from jax.experimental.pallas import tpu as pltpu
from jax.sharding import PartitionSpec as P

F32 = jnp.float32
BF16 = jnp.bfloat16
GELU_SCALE = 0.7978845608028654
GELU_CUBIC = 0.044715
COT_OVER_FS = False
TIED = True


def contract(left, right, dims, precision=None):
    return lax.dot_general(
        left, right, ((dims[:1], dims[1:]), ((), ())), precision=precision, preferred_element_type=F32
    )


def tile_of(size, wanted):
    return wanted if size % wanted == 0 else size


def chunk_of(rows):
    return 64 if rows % 64 == 0 else rows


def in_hbm(value):
    return pltpu.with_memory_space_constraint(value, pltpu.HBM)


def copies_over(vector, axis):
    count = lax.axis_size(axis)
    spread = jnp.broadcast_to(vector[None], (count,) + vector.shape)
    return jnp.sum(lax.all_to_all(spread, axis, split_axis=0, concat_axis=0, tiled=True), axis=0)


def call(kernel, grid, in_specs, out_specs, out_shape, scratch=(), flops=0):
    return pl.pallas_call(
        kernel,
        grid=grid,
        in_specs=in_specs,
        out_specs=out_specs,
        out_shape=out_shape,
        scratch_shapes=scratch,
        cost_estimate=pl.CostEstimate(flops=flops, transcendentals=0, bytes_accessed=flops // 256),
        compiler_params=pltpu.CompilerParams(
            dimension_semantics=("arbitrary",), vmem_limit_bytes=48 * 1024 * 1024
        ),
    )


def shifted_back(ref, start, rows, reach):
    current = ref[start : start + rows, :].astype(F32)
    if start == 0:
        before = jnp.zeros((8, current.shape[1]), F32)
    else:
        before = ref[start - 16 : start, :].astype(F32)[8:]
    joined = jnp.concatenate([before, current], 0)
    return [joined[8 - reach + k : 8 - reach + k + rows] for k in range(reach)] + [current]


def forward_kernel(places, *refs, pieces):
    conv_act, conv_val, bias_act, bias_val, mixed, slope, gate, up_act, up_val = refs[2 * pieces :]
    for index in range(pieces):
        count = refs[index].shape[0]
        start = pl.multiple_of(places[index] * count, count)
        up_act[pl.ds(start, count), :] = refs[index][...]
        up_val[pl.ds(start, count), :] = refs[pieces + index][...]
    total = up_act.shape[0]
    reach = conv_act.shape[0] - 1
    rows = chunk_of(total)

    def conv(ref, taps, bias, start):
        value = bias[...].astype(F32)
        weights = taps[...].astype(F32)
        for k, shifted in enumerate(shifted_back(ref, start, rows, reach)):
            value = value + weights[k : k + 1] * shifted
        return value

    for start in range(0, total, rows):
        here = slice(start, start + rows)
        act = conv(up_act, conv_act, bias_act, start)
        val = conv(up_val, conv_val, bias_val, start)
        square = act * act
        bent = jnp.tanh(act * (GELU_SCALE + (GELU_SCALE * GELU_CUBIC) * square))
        half = 0.5 + 0.5 * bent
        gelu = act * half
        inner = GELU_SCALE + (3.0 * GELU_SCALE * GELU_CUBIC) * square
        back = half + 0.5 * act * (1.0 - bent * bent) * inner
        mixed[here, :] = (gelu * val).astype(BF16)
        slope[here, :] = back * val
        gate[here, :] = gelu


def backward_kernel(
    core, mine, theirs, slope, gate, up_act, up_val, conv_act, conv_val, w_act, w_val,
    grad_act, grad_val, stats, partial, acc, *, tp_count, fs_count,
):
    total = up_act.shape[0]
    half = total // 2
    reach = conv_act.shape[0] - 1
    rows = chunk_of(half)
    first = core[0] == 0

    def mixed_grad(start, count):
        low = start < half
        at = slice(start % half, start % half + count)
        own, other = mine[at, :], theirs[at, :]
        own, other = own.astype(F32), other.astype(F32)
        return jnp.where(first == low, own, other)

    weights = (conv_act[...].astype(F32), conv_val[...].astype(F32))
    sums = [[None] * (reach + 2), [None] * (reach + 2)]

    def fold(value):
        if rows % 8 == 0:
            return jnp.sum(value.reshape(rows // 8, 8, value.shape[1]), axis=0)
        return jnp.sum(value, axis=0, keepdims=True)

    for start in range(0, total, rows):
        here = slice(start, start + rows)
        grad = mixed_grad(start, rows)
        last = start + rows >= total
        if not last:
            grad_next = mixed_grad(start + rows, 16)[:8]
        for role, (factor, up, out) in enumerate(
            ((slope, up_act, grad_act), (gate, up_val, grad_val))
        ):
            pre = grad * factor[here, :]
            if last:
                after = jnp.zeros((8, pre.shape[1]), F32)
            else:
                after = grad_next * factor[start + rows : start + rows + 8, :]
            joined = jnp.concatenate([pre, after], 0)
            source = up[here, :].astype(F32)
            value = None
            for k in range(reach + 1):
                ahead = reach - k
                moved = joined[ahead : ahead + rows] if ahead else pre
                term = weights[role][k : k + 1] * moved
                value = term if value is None else value + term
                add = fold(moved * source)
                sums[role][k] = add if sums[role][k] is None else sums[role][k] + add
            add = fold(pre)
            sums[role][-1] = add if sums[role][-1] is None else sums[role][-1] + add
            out[here, :] = value.astype(BF16)
    lines = [jnp.sum(entry, axis=0, keepdims=True) for role in sums for entry in role]
    for index, line in enumerate(lines):
        stats[index : index + 1, :] = line

    product = contract(grad_act[...], w_act[...], (1, 1)) + contract(
        grad_val[...], w_val[...], (1, 1)
    )
    step = pl.program_id(0)

    @pl.when(step == 0)
    def _():
        acc[...] = product

    @pl.when(step > 0)
    def _():
        acc[...] += product

    @pl.when(step == pl.num_programs(0) - 1)
    def _():
        shard = total // (tp_count * fs_count)
        for f in range(fs_count):
            for i in range(tp_count):
                start = (i * fs_count + f) * shard
                partial[f, i * shard : (i + 1) * shard, :] = acc[start : start + shard, :].astype(BF16)


def weight_kernel(left, *refs):
    count = len(refs) // 3
    for right, out, squares in zip(refs[:count], refs[count : 2 * count], refs[2 * count :]):
        value = contract(left[...], right[...], (0, 0))
        out[...] = value
        value = value * value
        width = value.shape[1]
        if width % 128 == 0:
            value = functools.reduce(
                jnp.add, [value[:, at : at + 128] for at in range(0, width, 128)]
            )
        ones = jnp.ones((8, value.shape[1]), F32)
        squares[...] = contract(ones, value, (1, 1), lax.Precision.HIGHEST)[:1]


def weight_grads(left, rights):
    rows, height = left.shape
    tile = tile_of(height, 256)
    width = rights[0].shape[1]
    count = len(rights)
    out = call(
        weight_kernel,
        (height // tile,),
        [pl.BlockSpec((rows, tile), lambda i: (0, i))]
        + [pl.BlockSpec((rows, width), lambda i: (0, 0))] * count,
        [pl.BlockSpec((tile, width), lambda i: (i, 0))] * count
        + [pl.BlockSpec((1, tile), lambda i: (0, i))] * count,
        [pltpu.HBM((height, width), F32)] * count
        + [jax.ShapeDtypeStruct((1, height), F32)] * count,
        flops=2 * rows * height * width * count,
    )(in_hbm(left), *[in_hbm(right) for right in rights])
    return out[:count], [entry.reshape(height) for entry in out[count:]]


def per_device(
    hidden_in,
    up_act,
    up_val,
    cotangent,
    w_act,
    w_val,
    w_down,
    conv_act,
    conv_val,
    bias_act,
    bias_val,
):
    local_rows = cotangent.shape[0]
    tap_count = conv_act.shape[0]
    tp_count = lax.axis_size("tp")
    fs_count = lax.axis_size("fs")
    chips = tp_count // 2
    total = local_rows * tp_count
    half = total // 2
    units = up_act.shape[1]
    width = w_act.shape[0]
    core = lax.axis_index("tp") % 2
    swap_cores = [(i, i ^ 1) for i in range(tp_count)]

    shard = local_rows // fs_count
    if COT_OVER_FS:
        own_rows = lax.dynamic_slice_in_dim(cotangent, lax.axis_index("fs") * shard, shard, 0)
        own_rows = jnp.transpose(own_rows.reshape(shard, tp_count, width), (1, 0, 2))
        own_rows = lax.all_to_all(own_rows, "tp", split_axis=0, concat_axis=0, tiled=True)
        cot_columns = lax.all_gather(own_rows, "fs", axis=0)
        cot_columns = jnp.transpose(cot_columns, (1, 0, 2, 3)).reshape(total, width)
    else:
        cot_blocks = jnp.transpose(cotangent.reshape(local_rows, tp_count, width), (1, 0, 2))
        cot_columns = lax.all_to_all(cot_blocks, "tp", split_axis=0, concat_axis=0, tiled=True)
        cot_columns = cot_columns.reshape(total, width)
        if TIED:
            cot_columns, up_act, up_val = lax.optimization_barrier((cot_columns, up_act, up_val))
    place = lax.axis_index("tp").astype(jnp.int32)
    if chips == 2:
        swap_chips = [(i, (i + 2) % tp_count) for i in range(tp_count)]
        ups = (up_act, up_val)
        across = [lax.ppermute(entry, "tp", swap_chips) for entry in ups]
        beside = [lax.ppermute(entry, "tp", swap_cores) for entry in ups]
        corner = [lax.ppermute(entry, "tp", swap_cores) for entry in across]
        gathered = [[ups[r], beside[r], across[r], corner[r]] for r in range(2)]
        places = jnp.stack([place, place ^ 1, place ^ 2, place ^ 3])
    else:
        gathered = [[lax.all_gather(entry, "tp", axis=0, tiled=True)] for entry in (up_act, up_val)]
        places = jnp.zeros((1,), jnp.int32)
    pieces = len(gathered[0])

    tile = tile_of(units, 256)
    column = pl.BlockSpec((total, tile), lambda i: (0, i))
    taps_spec = pl.BlockSpec((tap_count, tile), lambda i: (0, i))
    line_spec = pl.BlockSpec((1, tile), lambda i: (0, i))
    piece = pl.BlockSpec((total // pieces, tile), lambda i: (0, i))
    mixed, slope, gate, all_act, all_val = call(
        functools.partial(forward_kernel, pieces=pieces),
        (units // tile,),
        [pl.BlockSpec(memory_space=pltpu.SMEM)]
        + [piece] * (2 * pieces)
        + [taps_spec, taps_spec, line_spec, line_spec],
        [column] * 5,
        [pltpu.HBM((total, units), dtype) for dtype in (BF16, F32, F32, BF16, BF16)],
        flops=60 * total * units,
    )(
        places,
        *[in_hbm(entry) for entry in gathered[0] + gathered[1]],
        conv_act,
        conv_val,
        bias_act.reshape(1, units),
        bias_val.reshape(1, units),
    )

    away = contract(
        lax.dynamic_slice_in_dim(cot_columns, (1 - core) * half, half, 0), w_down, (1, 1)
    ).astype(BF16)
    arrived = lax.ppermute(away, "tp", swap_cores)
    kept = contract(lax.dynamic_slice_in_dim(cot_columns, core * half, half, 0), w_down, (1, 1))
    chip_sum = (kept + arrived.astype(F32)).astype(BF16)
    if chips == 2:
        other = lax.ppermute(chip_sum, "tp", swap_chips)
        mine = (chip_sum.astype(F32) + other.astype(F32)).astype(BF16)
    else:
        groups = [list(range(c, tp_count, 2)) for c in range(2)]
        parts = lax.all_gather(chip_sum, "tp", axis=0, axis_index_groups=groups)
        mine = jnp.sum(parts.astype(F32), axis=0).astype(BF16)
    theirs = lax.ppermute(mine, "tp", swap_cores)

    (grad_w_down,), (down_squares,) = weight_grads(mixed, (cot_columns,))

    half_spec = pl.BlockSpec((half, tile), lambda i: (0, i))
    weight_spec = pl.BlockSpec((width, tile), lambda i: (0, i))
    stat_count = 2 * (tap_count + 1)
    grad_act, grad_val, stats, partial = call(
        functools.partial(backward_kernel, tp_count=tp_count, fs_count=fs_count),
        (units // tile,),
        [pl.BlockSpec(memory_space=pltpu.SMEM)]
        + [half_spec] * 2
        + [column] * 4
        + [taps_spec] * 2
        + [weight_spec] * 2,
        [
            column,
            column,
            pl.BlockSpec((stat_count, tile), lambda i: (0, i)),
            pl.BlockSpec((fs_count, tp_count * shard, width), lambda i: (0, 0, 0)),
        ],
        [
            pltpu.HBM((total, units), BF16),
            pltpu.HBM((total, units), BF16),
            jax.ShapeDtypeStruct((stat_count, units), F32),
            pltpu.HBM((fs_count, tp_count * shard, width), BF16),
        ],
        scratch=[pltpu.VMEM((total, width), F32)],
        flops=4 * total * units * width,
    )(
        core.reshape(1).astype(jnp.int32),
        in_hbm(mine),
        in_hbm(theirs),
        in_hbm(slope),
        in_hbm(gate),
        in_hbm(all_act),
        in_hbm(all_val),
        conv_act,
        conv_val,
        in_hbm(w_act),
        in_hbm(w_val),
    )
    terms = lax.all_to_all(partial, "fs", split_axis=0, concat_axis=0, tiled=True)
    (grad_w_act, grad_w_val), (act_squares, val_squares) = weight_grads(
        hidden_in, (grad_act, grad_val)
    )
    taps_act, sums_act = stats[:tap_count], stats[tap_count]
    taps_val, sums_val = stats[tap_count + 1 : 2 * tap_count + 1], stats[2 * tap_count + 1]
    tap_squares = jnp.stack(
        [jnp.sum(taps_act * taps_act, axis=1), jnp.sum(taps_val * taps_val, axis=1)], 0
    )
    rows_down = copies_over(down_squares, "tp")
    lines = jnp.concatenate([act_squares, val_squares, tap_squares.reshape(-1)])
    lines = copies_over(lines, "fs")
    rows_act, rows_val = lines[:width], lines[width : 2 * width]
    conv_rows = lines[2 * width :].reshape(tap_squares.shape)
    summed = jnp.sum(terms.astype(F32), axis=0).astype(BF16).reshape(tp_count, shard, width)
    blocks = lax.all_to_all(summed, "tp", split_axis=0, concat_axis=0, tiled=True)
    grad_input = jnp.transpose(blocks, (1, 0, 2)).reshape(shard, tp_count * width)
    return (
        grad_input,
        grad_w_act,
        grad_w_val,
        grad_w_down,
        taps_act,
        taps_val,
        sums_act,
        sums_val,
        rows_act,
        rows_val,
        rows_down,
        conv_rows,
    )


def solution(mesh):
    return jax.shard_map(
        per_device,
        mesh=mesh,
        in_specs=(
            P(None, "tp"),
            P("tp", "fs"),
            P("tp", "fs"),
            P("tp", None),
            P("tp", "fs"),
            P("tp", "fs"),
            P("fs", "tp"),
            P(None, "fs"),
            P(None, "fs"),
            P("fs"),
            P("fs"),
        ),
        out_specs=(
            P(("tp", "fs"), None),
            P("tp", "fs"),
            P("tp", "fs"),
            P("fs", "tp"),
            P(None, "fs"),
            P(None, "fs"),
            P("fs"),
            P("fs"),
            P("tp"),
            P("tp"),
            P("fs"),
            P(),
        ),
        check_vma=False,
    )
```
